32 devices in a mesh: st: 16 (over z, y, x), tp: 2 (over core).
Axes of the slice: x: 2, y: 2, z: 4, core: 2. Of those that a mesh axis runs over, the one named last changes fastest.
Arguments:
- tokens: bfloat16 [16384, 2048], P('st', 'tp'), may hold values from -6 to 6
- passage_ids: int32 [256, 2], P('st'), may hold values from 0 to 255, as said below
- passage_store: bfloat16 [256, 64, 2048], P('st'), may hold values from -6 to 6
- norm_gain: bfloat16 [2048], replicated, may hold values from 0.099609375 to 1.8984375
- conv_value_weight: bfloat16 [2048, 1536], P(None, 'tp'), may hold values from -0.125 to 0.125
- conv_gate_weight: bfloat16 [2048, 1536], P(None, 'tp'), may hold values from -0.125 to 0.125
- conv_weight: bfloat16 [31, 1536], P(None, 'tp'), may hold values from -1 to 1
- ln_gain: bfloat16 [1536], P('tp'), may hold values from 0.099609375 to 1.8984375
- query_weight: bfloat16 [2048, 512], P(None, 'tp'), may hold values from -0.125 to 0.125
- query_gain: bfloat16 [512], P('tp'), may hold values from 0.5 to 10
- passage_gain: bfloat16 [2048], replicated, may hold values from 0.099609375 to 1.8984375
- key_weight: bfloat16 [2048, 512], P(None, 'tp'), may hold values from -0.125 to 0.125
- value_weight: bfloat16 [2048, 512], P(None, 'tp'), may hold values from -0.125 to 0.125
- key_gain: bfloat16 [512], P('tp'), may hold values from 0.5 to 10
- memory_gate: bfloat16 [512], P('tp'), may hold values from 0.29882812 to 1.5
- conv_out_weight: bfloat16 [1536, 2048], P('tp'), may hold values from -0.125 to 0.125
- memory_out_weight: bfloat16 [512, 2048], P('tp'), may hold values from -0.125 to 0.125
Outputs:
- layer_out: bfloat16 [16384, 2048], P(('st', 'tp'))
The draws below stay inside these ranges and needn't reach their ends.
Inputs may be any that keep to these rules, and one draw needn't show every extreme that they name: The owner of passage p is p // 16. Among the 32 entries of the rows of passage_ids that lie on one index of st (aligned runs of 16 rows, that is the blocks of one index of st), no owner is named more than 4 times, and in every such run some owner is named exactly 4 times.
All inputs are finite; a program needn't handle non-finite values.
Results may differ from the reference program's by a relative error of at most 0.008.
The reference program's roundings to bfloat16 on the way count: a program that leaves them out, or rounds other values in their place, can miss the bound.
Values may be sent and summed in bfloat16 or wider, within the bound.
A program may use at most 192 MiB of HBM per device.

```python
import jax
import jax.numpy as jnp
from jax import lax

D = 2048
C_A = 1536
MEM_HEADS = 8
MEM_HD = 64
MEM_W = 512
KW = 31
TOK_DEV = 1024
SEQS_DEV = 2
SEQ_LEN = 512
BLOCK = 64
PASS = 2
PLEN = 64
PASS_DEV = 16
TOKENS = 16384
BLOCKS = 256
PASSAGES = 256
N_ST = 16
N_TP = 2


def draw_passage_ids(key, part):
    owner_count = PASSAGES // PASS_DEV
    blocks_each = BLOCKS // owner_count
    request_count = blocks_each * PASS
    most_each = max(1, 2 * request_count // owner_count)
    slot_count = owner_count * most_each
    popular_key, hot_key, device_key = jax.random.split(jax.random.fold_in(key, 3), 3)
    popular = jax.random.randint(popular_key, (owner_count,), 0, 256)
    popular = popular * popular
    hot_owner = jax.random.randint(hot_key, (), 0, owner_count)
    slot_range = jnp.arange(slot_count, dtype=jnp.int32)
    slot_owner = slot_range // most_each
    first_slot = slot_range % most_each == 0

    def one_device(device):
        score_key, local_key, other_key, order_key = jax.random.split(jax.random.fold_in(device_key, device), 4)
        before = (device + owner_count - 1) % owner_count
        across = (device + owner_count // 2) % owner_count
        forced = (slot_owner == hot_owner) | first_slot & ((slot_owner == before) | (slot_owner == across))
        scores = jax.random.randint(score_key, (slot_count,), 0, 1 << 16) + popular[slot_owner] + jnp.where(forced, 1 << 18, 0)
        _, chosen = lax.top_k(scores * slot_count + slot_range, request_count)
        local_index = jnp.minimum(jax.random.randint(local_key, (request_count,), 0, PASS_DEV), jax.random.randint(other_key, (request_count,), 0, PASS_DEV))
        order = jax.random.permutation(order_key, request_count)
        picked = chosen // most_each * PASS_DEV + local_index
        return picked[order].reshape(blocks_each, PASS)
    return jax.vmap(one_device)(jnp.arange(owner_count, dtype=jnp.int32)).reshape(BLOCKS, PASS).astype(jnp.int32)


def gain_law(key):
    return jax.random.uniform(key, (MEM_W,), jnp.float32, 0.5, 2.5)


def draw_query_gain(key, part):
    return gain_law(jax.random.fold_in(key, 11)).astype(jnp.bfloat16)


def draw_key_gain(key, part):
    return gain_law(jax.random.fold_in(key, 17)).astype(jnp.bfloat16)


def draw_conv_weight(key, part):
    base = jax.random.truncated_normal(jax.random.fold_in(key, 23), -3.0, 3.0, (KW, C_A), jnp.float32)
    channel_scale = jnp.where(jnp.arange(C_A) < C_A // 2, 2.0, 0.6) * KW ** (-0.5)
    return jnp.clip(base * channel_scale[None, :], -1.0, 1.0).astype(jnp.bfloat16)


def shard_levels(key, shape, shards, low, largest):
    gain, own = 1.0, jax.random.fold_in(key, 6)
    for dim, blocks in shards:
        draws = jnp.exp(jax.random.uniform(jax.random.fold_in(own, dim), (blocks,), jnp.float32, low / len(shards), largest / len(shards)))
        gain = gain * jnp.repeat(draws, shape[dim] // blocks).reshape([-1 if axis == dim else 1 for axis in range(len(shape))])
    return gain


def gaussian(key, shape, spread, reach, shards=(), kind=jnp.bfloat16):
    array = jax.random.normal(key, shape, jnp.float32) * spread
    if len(shards) > 0:
        array = shard_levels(key, shape, shards, -0.22, 0.18) * array
    return jnp.clip(array, min=-reach, max=reach).astype(kind)


def setup_inputs(seed: int = 0) -> dict:
    streams_of = jax.random.split(jax.random.key(seed), 18)
    tokens = gaussian(streams_of[0], (TOKENS, D), 1.0, 6.0, ((0, 16), (1, 2)))
    passage_ids = draw_passage_ids(jax.random.fold_in(streams_of[17], 71), 0)
    passage_store = gaussian(streams_of[2], (PASSAGES, PLEN, D), 1.0, 6.0, ((0, 16),))
    norm_gain = jnp.clip(1.0 + 0.18 * jax.random.normal(streams_of[3], (D,), jnp.float32), 0.099609375, 1.8984375).astype(jnp.bfloat16)
    conv_value_weight = gaussian(streams_of[4], (D, C_A), D ** -0.5, 0.125, ((1, 2),))
    conv_gate_weight = gaussian(streams_of[5], (D, C_A), D ** -0.5, 0.125, ((1, 2),))
    conv_weight = draw_conv_weight(jax.random.fold_in(streams_of[17], 71), 0)
    ln_gain = jnp.clip(1.0 + 0.18 * jax.random.normal(streams_of[7], (C_A,), jnp.float32), 0.099609375, 1.8984375).astype(jnp.bfloat16)
    query_weight = gaussian(streams_of[8], (D, MEM_W), D ** -0.5, 0.125, ((1, 2),))
    query_gain = draw_query_gain(jax.random.fold_in(streams_of[17], 71), 0)
    passage_gain = jnp.clip(1.0 + 0.18 * jax.random.normal(streams_of[10], (D,), jnp.float32), 0.099609375, 1.8984375).astype(jnp.bfloat16)
    key_weight = gaussian(streams_of[11], (D, MEM_W), D ** -0.5, 0.125, ((1, 2),))
    value_weight = gaussian(streams_of[12], (D, MEM_W), D ** -0.5, 0.125, ((1, 2),))
    key_gain = draw_key_gain(jax.random.fold_in(streams_of[17], 71), 0)
    memory_gate = jnp.clip(0.29882812 + 1.2011719 * jax.random.uniform(streams_of[14], (MEM_W,), jnp.float32) ** shard_levels(streams_of[14], (MEM_W,), ((0, 2),), -0.2, 0.2), 0.29882812, 1.5).astype(jnp.bfloat16)
    conv_out_weight = gaussian(streams_of[15], (C_A, D), (C_A + MEM_W) ** -0.5, 0.125, ((0, 2),))
    memory_out_weight = gaussian(streams_of[16], (MEM_W, D), (C_A + MEM_W) ** -0.5, 0.125, ((0, 2),))
    return {"tokens": tokens, "passage_ids": passage_ids, "passage_store": passage_store, "norm_gain": norm_gain, "conv_value_weight": conv_value_weight, "conv_gate_weight": conv_gate_weight, "conv_weight": conv_weight, "ln_gain": ln_gain, "query_weight": query_weight, "query_gain": query_gain, "passage_gain": passage_gain, "key_weight": key_weight, "value_weight": value_weight, "key_gain": key_gain, "memory_gate": memory_gate, "conv_out_weight": conv_out_weight, "memory_out_weight": memory_out_weight}


NORM_EPS = 1e-06
LAYER_EPS = 1e-05

def row_norm(matrix, gain_row):
    widened = matrix.astype(jnp.float32)
    factor = lax.rsqrt(lax.optimization_barrier(jnp.mean(widened * widened, axis=-1, keepdims=True)) + NORM_EPS)
    return (widened * factor * gain_row.astype(jnp.float32)).astype(jnp.bfloat16)

def head_norm(product, gain_row, head_count):
    row_count = product.shape[0]
    split_heads = product.reshape(row_count, head_count, -1)
    factor = lax.rsqrt(lax.optimization_barrier(jnp.mean(split_heads * split_heads, axis=-1, keepdims=True)) + NORM_EPS)
    head_gains = gain_row.astype(jnp.float32).reshape(head_count, -1)
    return (split_heads * factor * head_gains).reshape(row_count, -1).astype(jnp.bfloat16)

def reference(tokens, passage_ids, passage_store, norm_gain, conv_value_weight, conv_gate_weight, conv_weight, ln_gain, query_weight, query_gain, passage_gain, key_weight, value_weight, key_gain, memory_gate, conv_out_weight, memory_out_weight):
    block_count = TOK_DEV // BLOCK
    token_groups = tokens.reshape(N_ST, TOK_DEV, D)
    id_groups = passage_ids.reshape(N_ST, block_count * PASS)
    taps = conv_weight.astype(jnp.float32)
    conv_part = C_A // N_TP
    head_part = MEM_W // N_TP

    def one_group(inputs):
        token_block, id_block = inputs
        normed_tokens = row_norm(token_block, norm_gain)
        up_value = jnp.dot(normed_tokens, conv_value_weight, preferred_element_type=jnp.float32)
        up_gate = jnp.dot(normed_tokens, conv_gate_weight, preferred_element_type=jnp.float32)
        gated_rows = (up_value * jax.nn.sigmoid(up_gate)).astype(jnp.bfloat16)
        sequences = gated_rows.astype(jnp.float32).reshape(SEQS_DEV, SEQ_LEN, C_A)
        padded = jnp.pad(sequences, ((0, 0), (KW - 1, 0), (0, 0)))
        filtered = jnp.zeros((SEQS_DEV, SEQ_LEN, C_A), jnp.float32)
        for tap in range(KW):
            filtered = filtered + taps[tap][None, None, :] * padded[:, tap:tap + SEQ_LEN, :]
        filtered = filtered.reshape(TOK_DEV, C_A)
        channel_mean = lax.optimization_barrier(jnp.sum(filtered, axis=-1, keepdims=True)) / C_A
        channel_var = lax.optimization_barrier(jnp.sum(filtered * filtered, axis=-1, keepdims=True)) / C_A - channel_mean * channel_mean
        scaled = (filtered - channel_mean) * lax.rsqrt(channel_var + LAYER_EPS) * ln_gain.astype(jnp.float32)
        conv_out = jax.nn.silu(scaled).astype(jnp.bfloat16)
        queries = head_norm(jnp.dot(normed_tokens, query_weight, preferred_element_type=jnp.float32), query_gain, MEM_HEADS)
        query_block = queries.reshape(block_count, BLOCK, MEM_HEADS, MEM_HD)
        fetched = passage_store[id_block].reshape(-1, D)
        normed_rows = row_norm(fetched, passage_gain)
        key_rows = head_norm(jnp.dot(normed_rows, key_weight, preferred_element_type=jnp.float32), key_gain, MEM_HEADS)
        value_rows = jnp.dot(normed_rows, value_weight, preferred_element_type=jnp.float32).astype(jnp.bfloat16)
        key_rows = key_rows.reshape(block_count, PASS * PLEN, MEM_HEADS, MEM_HD)
        value_rows = value_rows.reshape(block_count, PASS * PLEN, MEM_HEADS, MEM_HD)
        scores = jnp.einsum('nbhd,nkhd->nhbk', query_block.astype(jnp.float32), key_rows.astype(jnp.float32)) * MEM_HD ** (-0.5)
        row_max = lax.optimization_barrier(jnp.max(scores, axis=-1, keepdims=True))
        expanded = jnp.exp(scores - row_max)
        weights = (expanded / lax.optimization_barrier(jnp.sum(expanded, axis=-1, keepdims=True))).astype(jnp.bfloat16)
        attended = jnp.einsum('nhbk,nkhd->nbhd', weights.astype(jnp.float32), value_rows.astype(jnp.float32)).reshape(TOK_DEV, MEM_W)
        memory = (attended * jnp.tanh(memory_gate.astype(jnp.float32))).astype(jnp.bfloat16)
        running_sum = jnp.zeros((TOK_DEV, D), jnp.float32)
        for group_index in range(N_TP):
            conv_lo = group_index * conv_part
            head_lo = group_index * head_part
            partial_value = jnp.dot(conv_out[:, conv_lo:conv_lo + conv_part], conv_out_weight[conv_lo:conv_lo + conv_part], preferred_element_type=jnp.float32)
            partial_value = partial_value + jnp.dot(memory[:, head_lo:head_lo + head_part], memory_out_weight[head_lo:head_lo + head_part], preferred_element_type=jnp.float32)
            rounded = lax.optimization_barrier(partial_value.astype(jnp.bfloat16))
            running_sum = running_sum + rounded.astype(jnp.float32)
        return running_sum.astype(jnp.bfloat16)
    return lax.map(one_group, (token_groups, id_groups)).reshape(-1, D)
```

```python
import functools

import jax
import jax.numpy as jnp
from jax import lax
from jax.experimental import pallas as pl
from jax.experimental.pallas import tpu as pltpu
from jax.sharding import PartitionSpec as P

C_A = 1536
MEM_HD = 64
KW = 31
SEQS_DEV = 2


NORM_EPS = 1e-06
LAYER_EPS = 1e-05
VMEM_LIMIT = 60 * 1024 * 1024


def params():
    return pltpu.CompilerParams(
        dimension_semantics=("arbitrary",), vmem_limit_bytes=VMEM_LIMIT
    )


def head_norm(product, gain_row):
    lane = lax.broadcasted_iota(jnp.int32, product.shape, 1)
    squares = product * product
    scale = jnp.zeros_like(product)
    for head in range(product.shape[1] // MEM_HD):
        inside = (lane >= head * MEM_HD) & (lane < (head + 1) * MEM_HD)
        total = jnp.sum(jnp.where(inside, squares, 0.0), axis=-1, keepdims=True)
        scale = jnp.where(inside, lax.rsqrt(total * (1.0 / MEM_HD) + NORM_EPS), scale)
    return (product * scale * gain_row.astype(jnp.float32)).astype(jnp.bfloat16)


def dot32(left, right):
    return jnp.dot(left, right, preferred_element_type=jnp.float32)


def passage_kernel(rows_ref, gain_ref, key_w_ref, value_w_ref, key_gain_ref, out_ref):
    rows = rows_ref[...].astype(jnp.float32)
    factor = lax.rsqrt(jnp.mean(rows * rows, axis=-1, keepdims=True) + NORM_EPS)
    normed = (rows * factor * gain_ref[...].astype(jnp.float32)).astype(jnp.bfloat16)
    width = key_w_ref.shape[1]
    out_ref[:, :width] = head_norm(dot32(normed, key_w_ref[...]), key_gain_ref[...])
    out_ref[:, width:] = dot32(normed, value_w_ref[...]).astype(jnp.bfloat16)


def project_passages(rows, gain, key_weight, value_weight, key_gain):
    count, features = rows.shape
    width = key_weight.shape[1]
    tile = min(256, count)
    whole = lambda i: (0, 0)
    return pl.pallas_call(
        passage_kernel,
        grid=(count // tile,),
        in_specs=[
            pl.BlockSpec((tile, features), lambda i: (i, 0)),
            pl.BlockSpec((1, features), whole),
            pl.BlockSpec((features, width), whole),
            pl.BlockSpec((features, width), whole),
            pl.BlockSpec((1, width), whole),
        ],
        out_specs=pl.BlockSpec((tile, 2 * width), lambda i: (i, 0)),
        out_shape=jax.ShapeDtypeStruct((count, 2 * width), jnp.bfloat16),
        compiler_params=params(),
        cost_estimate=pl.CostEstimate(
            flops=4 * count * features * width, bytes_accessed=8 << 20, transcendentals=0
        ),
        name="project_passages",
    )(rows, gain[None, :], key_weight, value_weight, key_gain[None, :])


def token_kernel(
    index_ref,
    own_ref,
    other_ref,
    own_gain_ref,
    other_gain_ref,
    own_value_ref,
    other_value_ref,
    own_gate_ref,
    other_gate_ref,
    own_query_ref,
    other_query_ref,
    query_gain_ref,
    gated_ref,
    query_ref,
):
    own = own_ref[...].astype(jnp.float32)
    other = other_ref[...].astype(jnp.float32)
    total = jnp.sum(own * own, axis=-1, keepdims=True) + jnp.sum(
        other * other, axis=-1, keepdims=True
    )
    factor = lax.rsqrt(total * (0.5 / own.shape[1]) + NORM_EPS)
    own = (own * factor * own_gain_ref[...].astype(jnp.float32)).astype(jnp.bfloat16)
    other = (other * factor * other_gain_ref[...].astype(jnp.float32)).astype(jnp.bfloat16)
    query = dot32(own, own_query_ref[...]) + dot32(other, other_query_ref[...])
    query_ref[...] = head_norm(query, query_gain_ref[...])
    value = dot32(own, own_value_ref[...]) + dot32(other, other_value_ref[...])
    gate = dot32(own, own_gate_ref[...]) + dot32(other, other_gate_ref[...])
    gated_ref[...] = (value * jax.nn.sigmoid(gate)).astype(jnp.bfloat16)


def project_tokens(tp, own, other, gain, value_w, gate_w, query_w, query_gain):
    count, half = own.shape
    width, query_width = value_w.shape[1], query_w.shape[1]
    tile = min(256, count)
    rows = lambda i, s: (i, 0)
    mine = lambda i, s: (s[0], 0)
    theirs = lambda i, s: (1 - s[0], 0)
    return pl.pallas_call(
        token_kernel,
        grid_spec=pltpu.PrefetchScalarGridSpec(
            num_scalar_prefetch=1,
            grid=(count // tile,),
            in_specs=[
                pl.BlockSpec((tile, half), rows),
                pl.BlockSpec((tile, half), rows),
                pl.BlockSpec((1, half), lambda i, s: (0, s[0])),
                pl.BlockSpec((1, half), lambda i, s: (0, 1 - s[0])),
                pl.BlockSpec((half, width), mine),
                pl.BlockSpec((half, width), theirs),
                pl.BlockSpec((half, width), mine),
                pl.BlockSpec((half, width), theirs),
                pl.BlockSpec((half, query_width), mine),
                pl.BlockSpec((half, query_width), theirs),
                pl.BlockSpec((1, query_width), lambda i, s: (0, 0)),
            ],
            out_specs=[
                pl.BlockSpec((tile, width), rows),
                pl.BlockSpec((tile, query_width), rows),
            ],
        ),
        out_shape=(
            jax.ShapeDtypeStruct((count, width), jnp.bfloat16),
            jax.ShapeDtypeStruct((count, query_width), jnp.bfloat16),
        ),
        compiler_params=params(),
        cost_estimate=pl.CostEstimate(
            flops=4 * count * half * (2 * width + query_width),
            bytes_accessed=16 << 20,
            transcendentals=0,
        ),
        name="project_tokens",
    )(
        tp.reshape(1),
        own,
        other,
        gain[None, :],
        gain[None, :],
        value_w,
        value_w,
        gate_w,
        gate_w,
        query_w,
        query_w,
        query_gain[None, :],
    )


def attend_kernel(passes, slots_ref, query_ref, kv_ref, gate_ref, out_ref):
    width = query_ref.shape[1]
    heads = width // MEM_HD
    block = query_ref.shape[0] * passes // slots_ref.shape[0]
    head_of = lax.broadcasted_iota(jnp.int32, (heads * block, width), 1) // MEM_HD
    row_head = lax.broadcasted_iota(jnp.int32, (heads * block, width), 0) // block
    inside = head_of == row_head
    gate = jnp.tanh(gate_ref[...].astype(jnp.float32))

    @pl.loop(0, slots_ref.shape[0] // passes)
    def _(index):
        rows = pl.ds(pl.multiple_of(index * block, block), block)
        query = query_ref[rows, :]
        stacked = jnp.concatenate([query] * heads, axis=0)
        stacked = jnp.where(inside, stacked, jnp.zeros_like(stacked))
        read = [kv_ref[slots_ref[index * passes + part]] for part in range(passes)]
        keys = jnp.concatenate([part[:, :width] for part in read], axis=0)
        values = jnp.concatenate([part[:, width:] for part in read], axis=0)
        scores = lax.dot_general(
            stacked, keys, (((1,), (1,)), ((), ())), preferred_element_type=jnp.float32
        ) * MEM_HD ** (-0.5)
        expanded = jnp.exp(scores - jnp.max(scores, axis=-1, keepdims=True))
        weights = (expanded / jnp.sum(expanded, axis=-1, keepdims=True)).astype(jnp.bfloat16)
        mixed = jnp.where(inside, dot32(weights, values), 0.0)
        attended = mixed[:block]
        for head in range(1, heads):
            attended = attended + mixed[head * block : (head + 1) * block]
        out_ref[rows, :] = (attended * gate).astype(jnp.bfloat16)


def attend(slots, queries, received, gate, passes):
    vmem = pl.BlockSpec(memory_space=pltpu.VMEM)
    return pl.pallas_call(
        functools.partial(attend_kernel, passes),
        in_specs=[pl.BlockSpec(memory_space=pltpu.SMEM), vmem, vmem, vmem],
        out_specs=vmem,
        out_shape=jax.ShapeDtypeStruct(queries.shape, jnp.bfloat16),
        compiler_params=pltpu.CompilerParams(vmem_limit_bytes=VMEM_LIMIT),
        cost_estimate=pl.CostEstimate(
            flops=1 << 29, bytes_accessed=5 << 20, transcendentals=0
        ),
        name="attend",
    )(slots, queries, received, gate[None, :])


def body(
    tokens,
    passage_ids,
    passage_store,
    norm_gain,
    conv_value_weight,
    conv_gate_weight,
    conv_weight,
    ln_gain,
    query_weight,
    query_gain,
    passage_gain,
    key_weight,
    value_weight,
    key_gain,
    memory_gate,
    conv_out_weight,
    memory_out_weight,
):
    owner_count = lax.axis_size("st")
    tp = lax.axis_index("tp").astype(jnp.int32)
    swap = [(0, 1), (1, 0)]
    store_size, passage_len, feature_count = passage_store.shape
    flat_ids = passage_ids.reshape(-1)
    request_count = flat_ids.shape[0]
    most_each = max(1, 2 * request_count // owner_count)
    owner_index = flat_ids // store_size
    local_index = flat_ids % store_size
    owner_onehot = (
        owner_index[:, None] == jnp.arange(owner_count, dtype=jnp.int32)[None, :]
    ).astype(jnp.int32)
    earlier = jnp.cumsum(owner_onehot, axis=0) - owner_onehot
    slot_index = owner_index * most_each + jnp.sum(earlier * owner_onehot, axis=1)
    slot_onehot = (
        slot_index[:, None] == jnp.arange(owner_count * most_each, dtype=jnp.int32)[None, :]
    ).astype(jnp.int32)
    wanted = jnp.sum(slot_onehot * local_index[:, None], axis=0)
    asked_for = lax.all_to_all(
        wanted.reshape(owner_count, most_each), "st", split_axis=0, concat_axis=0, tiled=True
    ).reshape(-1)
    other_tokens = lax.ppermute(tokens, "tp", swap)
    projected = project_passages(
        passage_store.reshape(-1, feature_count), passage_gain, key_weight, value_weight, key_gain
    ).reshape(store_size, passage_len, -1)
    sent = jnp.take(projected, asked_for, axis=0, mode="clip")
    received = lax.all_to_all(sent, "st", split_axis=0, concat_axis=0, tiled=True)

    gated_rows, queries = project_tokens(
        tp,
        tokens,
        other_tokens,
        norm_gain,
        conv_value_weight,
        conv_gate_weight,
        query_weight,
        query_gain,
    )
    channel_count = conv_value_weight.shape[1]
    sequences = gated_rows.reshape(SEQS_DEV, -1, channel_count)
    filtered = lax.conv_general_dilated(
        sequences,
        conv_weight[:, None, :],
        (1,),
        [(KW - 1, 0)],
        dimension_numbers=("NWC", "WIO", "NWC"),
        feature_group_count=channel_count,
        preferred_element_type=jnp.float32,
    ).reshape(-1, channel_count)
    own_sums = jnp.stack([jnp.sum(filtered, axis=-1), jnp.sum(filtered * filtered, axis=-1)])
    stat_sums = own_sums + lax.ppermute(own_sums, "tp", swap)
    channel_mean = (stat_sums[0] / C_A)[:, None]
    channel_var = (stat_sums[1] / C_A)[:, None] - channel_mean * channel_mean
    scaled = (
        (filtered - channel_mean) * lax.rsqrt(channel_var + LAYER_EPS) * ln_gain.astype(jnp.float32)
    )
    conv_out = jax.nn.silu(scaled).astype(jnp.bfloat16)
    share = conv_out.shape[0] // 2
    conv_send = dot32(lax.dynamic_slice_in_dim(conv_out, (1 - tp) * share, share), conv_out_weight)
    conv_keep = dot32(lax.dynamic_slice_in_dim(conv_out, tp * share, share), conv_out_weight)

    memory = attend(slot_index, queries, received, memory_gate, passage_ids.shape[1])
    memory_send = lax.dynamic_slice_in_dim(memory, (1 - tp) * share, share)
    part_send = (conv_send + dot32(memory_send, memory_out_weight)).astype(jnp.bfloat16)
    part_back = lax.ppermute(part_send, "tp", swap)
    memory_keep = lax.dynamic_slice_in_dim(memory, tp * share, share)
    part_keep = (conv_keep + dot32(memory_keep, memory_out_weight)).astype(jnp.bfloat16)
    return (part_keep.astype(jnp.float32) + part_back.astype(jnp.float32)).astype(jnp.bfloat16)


def solution(mesh):
    return jax.shard_map(
        body,
        mesh=mesh,
        in_specs=(
            P("st", "tp"),
            P("st", None),
            P("st", None, None),
            P(),
            P(None, "tp"),
            P(None, "tp"),
            P(None, "tp"),
            P("tp"),
            P(None, "tp"),
            P("tp"),
            P(),
            P(None, "tp"),
            P(None, "tp"),
            P("tp"),
            P("tp"),
            P("tp", None),
            P("tp", None),
        ),
        out_specs=P(("st", "tp"), None),
        check_vma=False,
    )
```

```python
import functools

import jax
import jax.numpy as jnp
from jax import lax
from jax.experimental import pallas as pl
from jax.experimental.pallas import tpu as pltpu
from jax.sharding import PartitionSpec as P


C_A = 1536
MEM_HD = 64
SEQS_DEV = 2


NORM_EPS = 1e-06
LAYER_EPS = 1e-05
VMEM_LIMIT = 48 * 1024 * 1024


def params():
    return pltpu.CompilerParams(
        dimension_semantics=("arbitrary",), vmem_limit_bytes=VMEM_LIMIT
    )


def head_norm(product, gain_row):
    lane = lax.broadcasted_iota(jnp.int32, product.shape, 1)
    squares = product * product
    scale = jnp.zeros_like(product)
    for head in range(product.shape[1] // MEM_HD):
        inside = (lane >= head * MEM_HD) & (lane < (head + 1) * MEM_HD)
        total = jnp.sum(jnp.where(inside, squares, 0.0), axis=-1, keepdims=True)
        scale = jnp.where(inside, lax.rsqrt(total * (1.0 / MEM_HD) + NORM_EPS), scale)
    return (product * scale * gain_row.astype(jnp.float32)).astype(jnp.bfloat16)


def dot32(left, right):
    return jnp.dot(left, right, preferred_element_type=jnp.float32)


def passage_kernel(rows_ref, gain_ref, key_w_ref, value_w_ref, key_gain_ref, out_ref):
    rows = rows_ref[...].astype(jnp.float32)
    factor = lax.rsqrt(jnp.mean(rows * rows, axis=-1, keepdims=True) + NORM_EPS)
    normed = (rows * factor * gain_ref[...].astype(jnp.float32)).astype(jnp.bfloat16)
    width = key_w_ref.shape[1]
    out_ref[:, :width] = head_norm(dot32(normed, key_w_ref[...]), key_gain_ref[...])
    out_ref[:, width:] = dot32(normed, value_w_ref[...]).astype(jnp.bfloat16)


def project_passages(rows, gain, key_weight, value_weight, key_gain):
    count, features = rows.shape
    width = key_weight.shape[1]
    tile = min(256, count)
    whole = lambda i: (0, 0)
    return pl.pallas_call(
        passage_kernel,
        grid=(count // tile,),
        in_specs=[
            pl.BlockSpec((tile, features), lambda i: (i, 0)),
            pl.BlockSpec((1, features), whole),
            pl.BlockSpec((features, width), whole),
            pl.BlockSpec((features, width), whole),
            pl.BlockSpec((1, width), whole),
        ],
        out_specs=pl.BlockSpec((tile, 2 * width), lambda i: (i, 0)),
        out_shape=jax.ShapeDtypeStruct((count, 2 * width), jnp.bfloat16),
        compiler_params=params(),
        cost_estimate=pl.CostEstimate(
            flops=4 * count * features * width, bytes_accessed=8 << 20, transcendentals=0
        ),
        name="project_passages",
    )(rows, gain[None, :], key_weight, value_weight, key_gain[None, :])


def token_kernel(
    index_ref,
    own_ref,
    other_ref,
    own_gain_ref,
    other_gain_ref,
    own_value_ref,
    other_value_ref,
    own_gate_ref,
    other_gate_ref,
    own_query_ref,
    other_query_ref,
    query_gain_ref,
    gated_ref,
    query_ref,
):
    own = own_ref[...].astype(jnp.float32)
    other = other_ref[...].astype(jnp.float32)
    total = jnp.sum(own * own, axis=-1, keepdims=True) + jnp.sum(
        other * other, axis=-1, keepdims=True
    )
    factor = lax.rsqrt(total * (0.5 / own.shape[1]) + NORM_EPS)
    own = (own * factor * own_gain_ref[...].astype(jnp.float32)).astype(jnp.bfloat16)
    other = (other * factor * other_gain_ref[...].astype(jnp.float32)).astype(jnp.bfloat16)
    query = dot32(own, own_query_ref[...]) + dot32(other, other_query_ref[...])
    query_ref[...] = head_norm(query, query_gain_ref[...])
    value = dot32(own, own_value_ref[...]) + dot32(other, other_value_ref[...])
    gate = dot32(own, own_gate_ref[...]) + dot32(other, other_gate_ref[...])
    gated_ref[...] = (value * jax.nn.sigmoid(gate)).astype(jnp.bfloat16)


def project_tokens(tp, own, other, gain, value_w, gate_w, query_w, query_gain):
    count, half = own.shape
    width, query_width = value_w.shape[1], query_w.shape[1]
    tile = min(256, count)
    rows = lambda i, s: (i, 0)
    mine = lambda i, s: (s[0], 0)
    theirs = lambda i, s: (1 - s[0], 0)
    return pl.pallas_call(
        token_kernel,
        grid_spec=pltpu.PrefetchScalarGridSpec(
            num_scalar_prefetch=1,
            grid=(count // tile,),
            in_specs=[
                pl.BlockSpec((tile, half), rows),
                pl.BlockSpec((tile, half), rows),
                pl.BlockSpec((1, half), lambda i, s: (0, s[0])),
                pl.BlockSpec((1, half), lambda i, s: (0, 1 - s[0])),
                pl.BlockSpec((half, width), mine),
                pl.BlockSpec((half, width), theirs),
                pl.BlockSpec((half, width), mine),
                pl.BlockSpec((half, width), theirs),
                pl.BlockSpec((half, query_width), mine),
                pl.BlockSpec((half, query_width), theirs),
                pl.BlockSpec((1, query_width), lambda i, s: (0, 0)),
            ],
            out_specs=[
                pl.BlockSpec((tile, width), rows),
                pl.BlockSpec((tile, query_width), rows),
            ],
        ),
        out_shape=(
            jax.ShapeDtypeStruct((count, width), jnp.bfloat16),
            jax.ShapeDtypeStruct((count, query_width), jnp.bfloat16),
        ),
        compiler_params=params(),
        cost_estimate=pl.CostEstimate(
            flops=4 * count * half * (2 * width + query_width),
            bytes_accessed=16 << 20,
            transcendentals=0,
        ),
        name="project_tokens",
    )(
        tp.reshape(1),
        own,
        other,
        gain[None, :],
        gain[None, :],
        value_w,
        value_w,
        gate_w,
        gate_w,
        query_w,
        query_w,
        query_gain[None, :],
    )


def pick_kernel(most, stages, halves, *refs):
    asked_ref, refs = refs[0], refs[1:]
    count = halves if halves else len(stages)
    blocks, outs = refs[:count], refs[count:]
    for mate, out_ref in enumerate(outs):
        for place, relative in enumerate(stages):
            for slot in range(most):
                wanted = asked_ref[mate, relative * most + slot]
                target = place * most + slot
                if halves:
                    split = blocks[0].shape[0]

                    @pl.when(wanted < split)
                    def _():
                        out_ref[target] = blocks[0][jnp.minimum(wanted, split - 1)]

                    @pl.when(wanted >= split)
                    def _():
                        out_ref[target] = blocks[1][jnp.maximum(wanted - split, 0)]

                else:
                    out_ref[target] = blocks[place][wanted]


def pick(asked, blocks, stages, halves, most):
    vmem = pl.BlockSpec(memory_space=pltpu.VMEM)
    mates = asked.shape[0]
    shape = (len(stages) * most,) + blocks[0].shape[1:]
    return pl.pallas_call(
        functools.partial(pick_kernel, most, stages, len(blocks) if halves else 0),
        in_specs=[pl.BlockSpec(memory_space=pltpu.SMEM)] + [vmem] * len(blocks),
        out_specs=[vmem] * mates,
        out_shape=[jax.ShapeDtypeStruct(shape, jnp.bfloat16)] * mates,
        compiler_params=pltpu.CompilerParams(vmem_limit_bytes=16 << 20),
        cost_estimate=pl.CostEstimate(
            flops=1 << 28, bytes_accessed=2 << 20, transcendentals=0
        ),
        name="pick",
    )(asked, *blocks)


def conv_kernel(rows_ref, taps_ref, out_ref, padded_ref):
    length, width = rows_ref.shape
    taps = taps_ref.shape[0]
    lead = -(-(taps - 1) // 8) * 8
    chunk = 64
    span = chunk + lead + 8
    padded_ref[:lead, :] = jnp.zeros((lead, width), jnp.float32)
    padded_ref[lead + length :, :] = jnp.zeros((8, width), jnp.float32)
    padded_ref[lead : lead + length, :] = rows_ref[...].astype(jnp.float32)
    weights = taps_ref[...].astype(jnp.float32)

    @pl.loop(0, length // chunk)
    def _(index):
        base = pl.multiple_of(index * chunk, chunk)
        window = padded_ref[pl.ds(base, span), :]
        total = jnp.zeros((chunk, width), jnp.float32)
        for shift in range(8):
            moved = window if shift == 0 else pltpu.roll(window, span - shift, 0)
            for start in range(0, lead + 1, 8):
                tap = start + shift - (lead - taps + 1)
                if 0 <= tap < taps:
                    total += weights[tap : tap + 1, :] * moved[start : start + chunk, :]
        out_ref[pl.ds(base, chunk), :] = total


def depthwise(rows, taps, sequences):
    count, channels = rows.shape
    length = count // sequences
    width = 256 if channels % 256 == 0 else channels
    lead = -(-(taps.shape[0] - 1) // 8) * 8
    return pl.pallas_call(
        conv_kernel,
        grid=(sequences, channels // width),
        in_specs=[
            pl.BlockSpec((length, width), lambda i, j: (i, j)),
            pl.BlockSpec((taps.shape[0], width), lambda i, j: (0, j)),
        ],
        out_specs=pl.BlockSpec((length, width), lambda i, j: (i, j)),
        out_shape=jax.ShapeDtypeStruct(rows.shape, jnp.float32),
        scratch_shapes=[pltpu.VMEM((lead + length + 8, width), jnp.float32)],
        compiler_params=pltpu.CompilerParams(
            dimension_semantics=("arbitrary", "arbitrary"), vmem_limit_bytes=16 << 20
        ),
        cost_estimate=pl.CostEstimate(
            flops=8 << 30, bytes_accessed=5 << 20, transcendentals=0
        ),
        name="depthwise",
    )(rows, taps)


def attend_kernel(passes, most, plan, slots_ref, query_ref, gate_ref, *refs):
    pieces, (out_ref, kv_ref, sems) = refs[:-3], refs[-3:]
    copies = []
    for number, (piece, start, slot) in enumerate(plan):
        copies.append(
            pltpu.make_async_copy(
                pieces[piece].at[pl.ds(start, most)],
                kv_ref.at[pl.ds(slot, most)],
                sems.at[number],
            )
        )
        copies[-1].start()
    width = query_ref.shape[1]
    heads = width // MEM_HD
    block = query_ref.shape[0] * passes // slots_ref.shape[0]
    head_of = lax.broadcasted_iota(jnp.int32, (heads * block, width), 1) // MEM_HD
    row_head = lax.broadcasted_iota(jnp.int32, (heads * block, width), 0) // block
    inside = head_of == row_head
    gate = jnp.tanh(gate_ref[...].astype(jnp.float32))
    for copy in copies:
        copy.wait()

    @pl.loop(0, slots_ref.shape[0] // passes, unroll=4)
    def _(index):
        rows = pl.ds(pl.multiple_of(index * block, block), block)
        query = query_ref[rows, :]
        stacked = jnp.concatenate([query] * heads, axis=0)
        stacked = jnp.where(inside, stacked, jnp.zeros_like(stacked))
        read = [kv_ref[slots_ref[index * passes + part]] for part in range(passes)]
        keys = jnp.concatenate([part[:, :width] for part in read], axis=0)
        values = jnp.concatenate([part[:, width:] for part in read], axis=0)
        scores = lax.dot_general(
            stacked, keys, (((1,), (1,)), ((), ())), preferred_element_type=jnp.float32
        ) * MEM_HD ** (-0.5)
        expanded = jnp.exp(scores - jnp.max(scores, axis=-1, keepdims=True))
        weights = (expanded / jnp.sum(expanded, axis=-1, keepdims=True)).astype(jnp.bfloat16)
        mixed = jnp.where(inside, dot32(weights, values), 0.0)
        attended = mixed[:block]
        for head in range(1, heads):
            attended = attended + mixed[head * block : (head + 1) * block]
        out_ref[rows, :] = (attended * gate).astype(jnp.bfloat16)


def attend(slots, queries, pieces, plan, most, gate, passes):
    vmem = pl.BlockSpec(memory_space=pltpu.VMEM)
    anywhere = pl.BlockSpec(memory_space=pl.ANY)
    return pl.pallas_call(
        functools.partial(attend_kernel, passes, most, plan),
        in_specs=[pl.BlockSpec(memory_space=pltpu.SMEM), vmem, vmem]
        + [anywhere] * len(pieces),
        out_specs=vmem,
        out_shape=jax.ShapeDtypeStruct(queries.shape, jnp.bfloat16),
        scratch_shapes=[
            pltpu.VMEM((len(plan) * most,) + pieces[0].shape[1:], jnp.bfloat16),
            pltpu.SemaphoreType.DMA((len(plan),)),
        ],
        compiler_params=pltpu.CompilerParams(vmem_limit_bytes=24 << 20),
        cost_estimate=pl.CostEstimate(
            flops=1 << 29, bytes_accessed=5 << 20, transcendentals=0
        ),
        name="attend",
    )(slots, queries, gate[None, :], *pieces)


def split_axis(count):
    plane = 1
    for size in range(1, count + 1):
        if count % size == 0 and size * size <= count:
            plane = size
    return count // plane, plane


def layer(
    tokens,
    passage_ids,
    passage_store,
    norm_gain,
    conv_value_weight,
    conv_gate_weight,
    conv_weight,
    ln_gain,
    query_weight,
    query_gain,
    passage_gain,
    key_weight,
    value_weight,
    key_gain,
    memory_gate,
    conv_out_weight,
    memory_out_weight,
):
    owner_count = lax.axis_size("st")
    me = lax.axis_index("st").astype(jnp.int32)
    tp = lax.axis_index("tp").astype(jnp.int32)
    swap = [(0, 1), (1, 0)]
    depth, plane = split_axis(owner_count)
    power = plane & (plane - 1) == 0
    store_size, passage_len, feature_count = passage_store.shape

    def mate_of(place, step):
        return place ^ step if power else (place + step) % plane

    def along_plane(value, step, back):
        pairs = [
            (z * plane + p, z * plane + mate_of(p, step))
            for z in range(depth)
            for p in range(plane)
        ]
        return lax.ppermute(value, "st", [(b, a) for a, b in pairs] if back else pairs)

    def along_depth(value, step):
        pairs = [(i, (i + step * plane) % owner_count) for i in range(owner_count)]
        return lax.ppermute(value, "st", pairs)

    other_tokens = lax.ppermute(tokens, "tp", swap)
    own_block = project_passages(
        passage_store.reshape(-1, feature_count), passage_gain, key_weight, value_weight, key_gain
    ).reshape(store_size, passage_len, -1)

    flat_ids = passage_ids.reshape(-1)
    request_count = flat_ids.shape[0]
    most_each = max(1, 2 * request_count // owner_count)
    owner_index = flat_ids // store_size
    local_index = flat_ids % store_size
    same = (owner_index[:, None] == owner_index[None, :]) & (
        jnp.arange(request_count)[:, None] > jnp.arange(request_count)[None, :]
    )
    rank = jnp.sum(same.astype(jnp.int32), axis=1)
    relative = (owner_index // plane - me // plane + depth) % depth
    mate_place, my_place = owner_index % plane, me % plane
    step_to = (mate_place ^ my_place) if power else (my_place - mate_place + plane) % plane
    slot_index = (relative * plane + step_to) * most_each + rank
    slot_onehot = (
        slot_index[:, None] == jnp.arange(owner_count * most_each, dtype=jnp.int32)[None, :]
    ).astype(jnp.int32)
    wanted = jnp.sum(slot_onehot * local_index[:, None], axis=0).reshape(depth, plane, most_each)
    asked = jnp.stack(
        [wanted[:, 0]] + [along_plane(wanted[:, step], step, True) for step in range(1, plane)]
    ).reshape(plane, depth * most_each)

    pieces, plan = [], []

    def deliver(blocks, stages, halves):
        picked = pick(asked, blocks, stages, halves, most_each)
        for step, part in enumerate(picked):
            for place, offset in enumerate(stages):
                plan.append(
                    (len(pieces), place * most_each, (offset * plane + step) * most_each)
                )
            pieces.append(part if step == 0 else along_plane(part, step, False))

    gated_rows, queries = project_tokens(
        tp,
        tokens,
        other_tokens,
        norm_gain,
        conv_value_weight,
        conv_gate_weight,
        query_weight,
        query_gain,
    )
    asked, gated_rows = lax.optimization_barrier((asked, gated_rows))
    deliver((own_block,), (0,), False)
    pieces[0], gated_rows = lax.optimization_barrier((pieces[0], gated_rows))
    filtered = depthwise(gated_rows, conv_weight, SEQS_DEV)

    rising, falling = own_block, own_block
    for hop in range(1, (depth - 1) // 2 + 1):
        rising, falling = along_depth(rising, 1), along_depth(falling, -1)
        rising, falling, filtered = lax.optimization_barrier((rising, falling, filtered))
        deliver((rising, falling), (depth - hop, hop), False)
    own_sums = jnp.stack([jnp.sum(filtered, axis=-1), jnp.sum(filtered * filtered, axis=-1)])
    stat_sums = own_sums + lax.ppermute(own_sums, "tp", swap)
    channel_mean = (stat_sums[0] / C_A)[:, None]
    channel_var = (stat_sums[1] / C_A)[:, None] - channel_mean * channel_mean
    scaled = (
        (filtered - channel_mean) * lax.rsqrt(channel_var + LAYER_EPS) * ln_gain.astype(jnp.float32)
    )
    conv_out = jax.nn.silu(scaled).astype(jnp.bfloat16)
    share = conv_out.shape[0] // 2
    conv_send = dot32(lax.dynamic_slice_in_dim(conv_out, (1 - tp) * share, share), conv_out_weight)
    conv_keep = dot32(lax.dynamic_slice_in_dim(conv_out, tp * share, share), conv_out_weight)
    if depth % 2 == 0:
        half = store_size // 2
        low, high = along_depth(rising[:half], 1), along_depth(falling[half:], -1)
        low, high, conv_send = lax.optimization_barrier((low, high, conv_send))
        deliver((low, high), (depth // 2,), True)

    memory = attend(
        slot_index, queries, pieces, tuple(plan), most_each, memory_gate, passage_ids.shape[1]
    )
    memory_send = lax.dynamic_slice_in_dim(memory, (1 - tp) * share, share)
    part_send = (conv_send + dot32(memory_send, memory_out_weight)).astype(jnp.bfloat16)
    part_back = lax.ppermute(part_send, "tp", swap)
    memory_keep = lax.dynamic_slice_in_dim(memory, tp * share, share)
    part_keep = (conv_keep + dot32(memory_keep, memory_out_weight)).astype(jnp.bfloat16)
    return (part_keep.astype(jnp.float32) + part_back.astype(jnp.float32)).astype(jnp.bfloat16)


def solution(mesh):
    return jax.shard_map(
        layer,
        mesh=mesh,
        in_specs=(
            P("st", "tp"),
            P("st", None),
            P("st", None, None),
            P(),
            P(None, "tp"),
            P(None, "tp"),
            P(None, "tp"),
            P("tp"),
            P(None, "tp"),
            P("tp"),
            P(),
            P(None, "tp"),
            P(None, "tp"),
            P("tp"),
            P("tp"),
            P("tp", None),
            P("tp", None),
        ),
        out_specs=P(("st", "tp"), None),
        check_vma=False,
    )
```

```python
import functools

import jax
import jax.numpy as jnp
from jax import lax
from jax.experimental import pallas as pl
from jax.experimental.pallas import tpu as pltpu
from jax.sharding import PartitionSpec as P


C_A = 1536
MEM_HD = 64
SEQS_DEV = 2


NORM_EPS = 1e-06
LAYER_EPS = 1e-05
VMEM_LIMIT = 60 * 1024 * 1024


def params():
    return pltpu.CompilerParams(
        dimension_semantics=("arbitrary",), vmem_limit_bytes=VMEM_LIMIT
    )


def head_norm(product, gain_row):
    lane = lax.broadcasted_iota(jnp.int32, product.shape, 1)
    squares = product * product
    scale = jnp.zeros_like(product)
    for head in range(product.shape[1] // MEM_HD):
        inside = (lane >= head * MEM_HD) & (lane < (head + 1) * MEM_HD)
        total = jnp.sum(jnp.where(inside, squares, 0.0), axis=-1, keepdims=True)
        scale = jnp.where(inside, lax.rsqrt(total * (1.0 / MEM_HD) + NORM_EPS), scale)
    return (product * scale * gain_row.astype(jnp.float32)).astype(jnp.bfloat16)


def dot32(left, right):
    return jnp.dot(left, right, preferred_element_type=jnp.float32)


def passage_kernel(rows_ref, gain_ref, key_w_ref, value_w_ref, key_gain_ref, out_ref):
    rows = rows_ref[...].astype(jnp.float32)
    factor = lax.rsqrt(jnp.mean(rows * rows, axis=-1, keepdims=True) + NORM_EPS)
    normed = (rows * factor * gain_ref[...].astype(jnp.float32)).astype(jnp.bfloat16)
    width = key_w_ref.shape[1]
    out_ref[:, :width] = head_norm(dot32(normed, key_w_ref[...]), key_gain_ref[...])
    out_ref[:, width:] = dot32(normed, value_w_ref[...]).astype(jnp.bfloat16)


def project_passages(rows, start, count, gain, key_weight, value_weight, key_gain):
    features = rows.shape[1]
    width = key_weight.shape[1]
    tile = min(256, count)
    first = start // tile
    whole = lambda i: (0, 0)
    return pl.pallas_call(
        passage_kernel,
        grid=(count // tile,),
        in_specs=[
            pl.BlockSpec((tile, features), lambda i: (i + first, 0)),
            pl.BlockSpec((1, features), whole),
            pl.BlockSpec((features, width), whole),
            pl.BlockSpec((features, width), whole),
            pl.BlockSpec((1, width), whole),
        ],
        out_specs=pl.BlockSpec((tile, 2 * width), lambda i: (i, 0)),
        out_shape=jax.ShapeDtypeStruct((count, 2 * width), jnp.bfloat16),
        compiler_params=params(),
        cost_estimate=pl.CostEstimate(
            flops=4 * count * features * width, bytes_accessed=8 << 20, transcendentals=0
        ),
        name="project_passages",
    )(rows, gain[None, :], key_weight, value_weight, key_gain[None, :])


def token_kernel(
    index_ref,
    own_ref,
    other_ref,
    own_gain_ref,
    other_gain_ref,
    own_value_ref,
    other_value_ref,
    own_gate_ref,
    other_gate_ref,
    own_query_ref,
    other_query_ref,
    query_gain_ref,
    gated_ref,
    query_ref,
):
    own = own_ref[...].astype(jnp.float32)
    other = other_ref[...].astype(jnp.float32)
    total = jnp.sum(own * own, axis=-1, keepdims=True) + jnp.sum(
        other * other, axis=-1, keepdims=True
    )
    factor = lax.rsqrt(total * (0.5 / own.shape[1]) + NORM_EPS)
    own = (own * factor * own_gain_ref[...].astype(jnp.float32)).astype(jnp.bfloat16)
    other = (other * factor * other_gain_ref[...].astype(jnp.float32)).astype(jnp.bfloat16)
    query = dot32(own, own_query_ref[...]) + dot32(other, other_query_ref[...])
    query_ref[...] = head_norm(query, query_gain_ref[...])
    value = dot32(own, own_value_ref[...]) + dot32(other, other_value_ref[...])
    gate = dot32(own, own_gate_ref[...]) + dot32(other, other_gate_ref[...])
    gated_ref[...] = (value * jax.nn.sigmoid(gate)).astype(jnp.bfloat16)


def project_tokens(tp, own, other, gain, value_w, gate_w, query_w, query_gain):
    count, half = own.shape
    width, query_width = value_w.shape[1], query_w.shape[1]
    tile = min(256, count)
    rows = lambda i, s: (i, 0)
    mine = lambda i, s: (s[0], 0)
    theirs = lambda i, s: (1 - s[0], 0)
    return pl.pallas_call(
        token_kernel,
        grid_spec=pltpu.PrefetchScalarGridSpec(
            num_scalar_prefetch=1,
            grid=(count // tile,),
            in_specs=[
                pl.BlockSpec((tile, half), rows),
                pl.BlockSpec((tile, half), rows),
                pl.BlockSpec((1, half), lambda i, s: (0, s[0])),
                pl.BlockSpec((1, half), lambda i, s: (0, 1 - s[0])),
                pl.BlockSpec((half, width), mine),
                pl.BlockSpec((half, width), theirs),
                pl.BlockSpec((half, width), mine),
                pl.BlockSpec((half, width), theirs),
                pl.BlockSpec((half, query_width), mine),
                pl.BlockSpec((half, query_width), theirs),
                pl.BlockSpec((1, query_width), lambda i, s: (0, 0)),
            ],
            out_specs=[
                pl.BlockSpec((tile, width), rows),
                pl.BlockSpec((tile, query_width), rows),
            ],
        ),
        out_shape=(
            jax.ShapeDtypeStruct((count, width), jnp.bfloat16),
            jax.ShapeDtypeStruct((count, query_width), jnp.bfloat16),
        ),
        compiler_params=params(),
        cost_estimate=pl.CostEstimate(
            flops=4 * count * half * (2 * width + query_width),
            bytes_accessed=16 << 20,
            transcendentals=0,
        ),
        name="project_tokens",
    )(
        tp.reshape(1),
        own,
        other,
        gain[None, :],
        gain[None, :],
        value_w,
        value_w,
        gate_w,
        gate_w,
        query_w,
        query_w,
        query_gain[None, :],
    )


def pick_kernel(most, stages, *refs):
    asked_ref, refs = refs[0], refs[1:]
    blocks, outs = refs[: 2 * len(stages)], refs[2 * len(stages) :]
    for mate, out_ref in enumerate(outs):
        for place, relative in enumerate(stages):
            low_ref, high_ref = blocks[2 * place], blocks[2 * place + 1]
            split = low_ref.shape[0]
            for slot in range(most):
                wanted = asked_ref[mate, relative * most + slot]
                target = place * most + slot

                @pl.when(wanted < split)
                def _(low_ref=low_ref, split=split, wanted=wanted, target=target):
                    out_ref[target] = low_ref[jnp.minimum(wanted, split - 1)]

                @pl.when(wanted >= split)
                def _(high_ref=high_ref, split=split, wanted=wanted, target=target):
                    out_ref[target] = high_ref[jnp.maximum(wanted - split, 0)]


def pick(asked, blocks, stages, most):
    vmem = pl.BlockSpec(memory_space=pltpu.VMEM)
    mates = asked.shape[0]
    shape = (len(stages) * most,) + blocks[0].shape[1:]
    return pl.pallas_call(
        functools.partial(pick_kernel, most, stages),
        in_specs=[pl.BlockSpec(memory_space=pltpu.SMEM)] + [vmem] * len(blocks),
        out_specs=[vmem] * mates,
        out_shape=[jax.ShapeDtypeStruct(shape, jnp.bfloat16)] * mates,
        compiler_params=pltpu.CompilerParams(vmem_limit_bytes=16 << 20),
        cost_estimate=pl.CostEstimate(
            flops=1 << 28, bytes_accessed=2 << 20, transcendentals=0
        ),
        name="pick",
    )(asked, *blocks)


def conv_kernel(rows_ref, taps_ref, out_ref, padded_ref):
    length, width = rows_ref.shape
    taps = taps_ref.shape[0]
    lead = -(-(taps - 1) // 8) * 8
    chunk = 64
    span = chunk + lead + 8
    padded_ref[:lead, :] = jnp.zeros((lead, width), jnp.float32)
    padded_ref[lead + length :, :] = jnp.zeros((8, width), jnp.float32)
    padded_ref[lead : lead + length, :] = rows_ref[...].astype(jnp.float32)
    weights = taps_ref[...].astype(jnp.float32)

    @pl.loop(0, length // chunk)
    def _(index):
        base = pl.multiple_of(index * chunk, chunk)
        window = padded_ref[pl.ds(base, span), :]
        total = jnp.zeros((chunk, width), jnp.float32)
        for shift in range(8):
            moved = window if shift == 0 else pltpu.roll(window, span - shift, 0)
            for start in range(0, lead + 1, 8):
                tap = start + shift - (lead - taps + 1)
                if 0 <= tap < taps:
                    total += weights[tap : tap + 1, :] * moved[start : start + chunk, :]
        out_ref[pl.ds(base, chunk), :] = total


def depthwise(rows, taps, sequences):
    count, channels = rows.shape
    length = count // sequences
    width = 256 if channels % 256 == 0 else channels
    lead = -(-(taps.shape[0] - 1) // 8) * 8
    return pl.pallas_call(
        conv_kernel,
        grid=(sequences, channels // width),
        in_specs=[
            pl.BlockSpec((length, width), lambda i, j: (i, j)),
            pl.BlockSpec((taps.shape[0], width), lambda i, j: (0, j)),
        ],
        out_specs=pl.BlockSpec((length, width), lambda i, j: (i, j)),
        out_shape=jax.ShapeDtypeStruct(rows.shape, jnp.float32),
        scratch_shapes=[pltpu.VMEM((lead + length + 8, width), jnp.float32)],
        compiler_params=pltpu.CompilerParams(
            dimension_semantics=("arbitrary", "arbitrary"), vmem_limit_bytes=16 << 20
        ),
        cost_estimate=pl.CostEstimate(
            flops=8 << 30, bytes_accessed=5 << 20, transcendentals=0
        ),
        name="depthwise",
    )(rows, taps)


def attend_kernel(passes, most, plan, slots_ref, query_ref, gate_ref, *refs):
    pieces, (out_ref, kv_ref, sems) = refs[:-3], refs[-3:]
    copies = []
    for number, (piece, start, slot) in enumerate(plan):
        copies.append(
            pltpu.make_async_copy(
                pieces[piece].at[pl.ds(start, most)],
                kv_ref.at[pl.ds(slot, most)],
                sems.at[number],
            )
        )
        copies[-1].start()
    width = query_ref.shape[1]
    heads = width // MEM_HD
    block = query_ref.shape[0] * passes // slots_ref.shape[0]
    head_of = lax.broadcasted_iota(jnp.int32, (heads * block, width), 1) // MEM_HD
    row_head = lax.broadcasted_iota(jnp.int32, (heads * block, width), 0) // block
    inside = head_of == row_head
    gate = jnp.tanh(gate_ref[...].astype(jnp.float32))
    for copy in copies:
        copy.wait()

    @pl.loop(0, slots_ref.shape[0] // passes, unroll=4)
    def _(index):
        rows = pl.ds(pl.multiple_of(index * block, block), block)
        query = query_ref[rows, :]
        stacked = jnp.concatenate([query] * heads, axis=0)
        stacked = jnp.where(inside, stacked, jnp.zeros_like(stacked))
        read = [kv_ref[slots_ref[index * passes + part]] for part in range(passes)]
        keys = jnp.concatenate([part[:, :width] for part in read], axis=0)
        values = jnp.concatenate([part[:, width:] for part in read], axis=0)
        scores = lax.dot_general(
            stacked, keys, (((1,), (1,)), ((), ())), preferred_element_type=jnp.float32
        ) * MEM_HD ** (-0.5)
        expanded = jnp.exp(scores - jnp.max(scores, axis=-1, keepdims=True))
        weights = (expanded / jnp.sum(expanded, axis=-1, keepdims=True)).astype(jnp.bfloat16)
        mixed = jnp.where(inside, dot32(weights, values), 0.0)
        attended = mixed[:block]
        for head in range(1, heads):
            attended = attended + mixed[head * block : (head + 1) * block]
        out_ref[rows, :] = (attended * gate).astype(jnp.bfloat16)


def attend(slots, queries, pieces, plan, most, gate, passes):
    vmem = pl.BlockSpec(memory_space=pltpu.VMEM)
    anywhere = pl.BlockSpec(memory_space=pl.ANY)
    return pl.pallas_call(
        functools.partial(attend_kernel, passes, most, plan),
        in_specs=[pl.BlockSpec(memory_space=pltpu.SMEM), vmem, vmem]
        + [anywhere] * len(pieces),
        out_specs=vmem,
        out_shape=jax.ShapeDtypeStruct(queries.shape, jnp.bfloat16),
        scratch_shapes=[
            pltpu.VMEM((len(plan) * most,) + pieces[0].shape[1:], jnp.bfloat16),
            pltpu.SemaphoreType.DMA((len(plan),)),
        ],
        compiler_params=pltpu.CompilerParams(vmem_limit_bytes=24 << 20),
        cost_estimate=pl.CostEstimate(
            flops=1 << 29, bytes_accessed=5 << 20, transcendentals=0
        ),
        name="attend",
    )(slots, queries, gate[None, :], *pieces)


def split_axis(count):
    plane = 1
    for size in range(1, count + 1):
        if count % size == 0 and size * size <= count:
            plane = size
    return count // plane, plane


def layer(
    tokens,
    passage_ids,
    passage_store,
    norm_gain,
    conv_value_weight,
    conv_gate_weight,
    conv_weight,
    ln_gain,
    query_weight,
    query_gain,
    passage_gain,
    key_weight,
    value_weight,
    key_gain,
    memory_gate,
    conv_out_weight,
    memory_out_weight,
):
    owner_count = lax.axis_size("st")
    me = lax.axis_index("st").astype(jnp.int32)
    tp = lax.axis_index("tp").astype(jnp.int32)
    swap = [(0, 1), (1, 0)]
    depth, plane = split_axis(owner_count)
    power = plane & (plane - 1) == 0
    store_size, passage_len, feature_count = passage_store.shape

    def mate_of(place, step):
        return place ^ step if power else (place + step) % plane

    def along_plane(value, step, back):
        pairs = [
            (z * plane + p, z * plane + mate_of(p, step))
            for z in range(depth)
            for p in range(plane)
        ]
        return lax.ppermute(value, "st", [(b, a) for a, b in pairs] if back else pairs)

    def along_depth(value, step):
        pairs = [(i, (i + step * plane) % owner_count) for i in range(owner_count)]
        return lax.ppermute(value, "st", pairs)

    other_tokens = lax.ppermute(tokens, "tp", swap)
    half = store_size // 2
    store_rows = passage_store.reshape(-1, feature_count)
    own_block = tuple(
        project_passages(
            store_rows,
            start * passage_len,
            half * passage_len,
            passage_gain,
            key_weight,
            value_weight,
            key_gain,
        ).reshape(half, passage_len, -1)
        for start in (0, half)
    )

    flat_ids = passage_ids.reshape(-1)
    request_count = flat_ids.shape[0]
    most_each = max(1, 2 * request_count // owner_count)
    owner_index = flat_ids // store_size
    local_index = flat_ids % store_size
    same = (owner_index[:, None] == owner_index[None, :]) & (
        jnp.arange(request_count)[:, None] > jnp.arange(request_count)[None, :]
    )
    rank = jnp.sum(same.astype(jnp.int32), axis=1)
    relative = (owner_index // plane - me // plane + depth) % depth
    mate_place, my_place = owner_index % plane, me % plane
    step_to = (mate_place ^ my_place) if power else (my_place - mate_place + plane) % plane
    slot_index = (relative * plane + step_to) * most_each + rank
    slot_onehot = (
        slot_index[:, None] == jnp.arange(owner_count * most_each, dtype=jnp.int32)[None, :]
    ).astype(jnp.int32)
    wanted = jnp.sum(slot_onehot * local_index[:, None], axis=0).reshape(depth, plane, most_each)
    asked = jnp.stack(
        [wanted[:, 0]] + [along_plane(wanted[:, step], step, True) for step in range(1, plane)]
    ).reshape(plane, depth * most_each)

    pieces, plan = [], []

    def deliver(blocks, stages):
        picked = pick(asked, blocks, stages, most_each)
        for step, part in enumerate(picked):
            for place, offset in enumerate(stages):
                plan.append(
                    (len(pieces), place * most_each, (offset * plane + step) * most_each)
                )
            pieces.append(part if step == 0 else along_plane(part, step, False))

    gated_rows, queries = project_tokens(
        tp,
        tokens,
        other_tokens,
        norm_gain,
        conv_value_weight,
        conv_gate_weight,
        query_weight,
        query_gain,
    )
    asked, gated_rows = lax.optimization_barrier((asked, gated_rows))
    deliver(own_block, (0,))
    pieces[0], gated_rows = lax.optimization_barrier((pieces[0], gated_rows))
    filtered = depthwise(gated_rows, conv_weight, SEQS_DEV)

    rising, falling = own_block, own_block
    for hop in range(1, (depth - 1) // 2 + 1):
        rising_low = along_depth(rising[0], 1)
        falling_high = along_depth(falling[1], -1)
        rising_high = along_depth(rising[1], 1)
        falling_low = along_depth(falling[0], -1)
        rising_high, falling_low, filtered = lax.optimization_barrier(
            (rising_high, falling_low, filtered)
        )
        rising, falling = (rising_low, rising_high), (falling_low, falling_high)
        deliver(rising + falling, (depth - hop, hop))
    own_sums = jnp.stack([jnp.sum(filtered, axis=-1), jnp.sum(filtered * filtered, axis=-1)])
    stat_sums = own_sums + lax.ppermute(own_sums, "tp", swap)
    channel_mean = (stat_sums[0] / C_A)[:, None]
    channel_var = (stat_sums[1] / C_A)[:, None] - channel_mean * channel_mean
    scaled = (
        (filtered - channel_mean) * lax.rsqrt(channel_var + LAYER_EPS) * ln_gain.astype(jnp.float32)
    )
    conv_out = jax.nn.silu(scaled).astype(jnp.bfloat16)
    share = conv_out.shape[0] // 2
    conv_send = dot32(lax.dynamic_slice_in_dim(conv_out, (1 - tp) * share, share), conv_out_weight)
    conv_keep = dot32(lax.dynamic_slice_in_dim(conv_out, tp * share, share), conv_out_weight)
    if depth % 2 == 0:
        low = along_depth(rising[0], 1)
        high = along_depth(falling[1], -1)
        low, high, conv_send = lax.optimization_barrier((low, high, conv_send))
        deliver((low, high), (depth // 2,))

    memory = attend(
        slot_index, queries, pieces, tuple(plan), most_each, memory_gate, passage_ids.shape[1]
    )
    memory_send = lax.dynamic_slice_in_dim(memory, (1 - tp) * share, share)
    part_send = (conv_send + dot32(memory_send, memory_out_weight)).astype(jnp.bfloat16)
    part_back = lax.ppermute(part_send, "tp", swap)
    memory_keep = lax.dynamic_slice_in_dim(memory, tp * share, share)
    part_keep = (conv_keep + dot32(memory_keep, memory_out_weight)).astype(jnp.bfloat16)
    return (part_keep.astype(jnp.float32) + part_back.astype(jnp.float32)).astype(jnp.bfloat16)


def solution(mesh):
    return jax.shard_map(
        layer,
        mesh=mesh,
        in_specs=(
            P("st", "tp"),
            P("st", None),
            P("st", None, None),
            P(),
            P(None, "tp"),
            P(None, "tp"),
            P(None, "tp"),
            P("tp"),
            P(None, "tp"),
            P("tp"),
            P(),
            P(None, "tp"),
            P(None, "tp"),
            P("tp"),
            P("tp"),
            P("tp", None),
            P("tp", None),
        ),
        out_specs=P(("st", "tp"), None),
        check_vma=False,
    )
```
